32 devices in a mesh: sp: 4 (over z), fs: 4 (over y, x), tp: 2 (over core).
Axes of the slice: x: 2, y: 2, z: 4, core: 2. Of those that a mesh axis runs over, the one named last changes fastest.
Arguments:
- tokens: bfloat16 [8, 768, 2048], P(('fs', 'tp'), 'sp'), may hold values from -6 to 6
- linear_query: bfloat16 [2048, 512], P(('sp', 'tp'), 'fs'), may hold values from -0.125 to 0.125
- linear_key: bfloat16 [2048, 512], P(('sp', 'tp'), 'fs'), may hold values from -0.125 to 0.125
- linear_decay: bfloat16 [2048, 512], P(('sp', 'tp'), 'fs'), may hold values from -0.25 to 0.25
- linear_value: bfloat16 [2048, 1024], P(('sp', 'tp'), 'fs'), may hold values from -0.125 to 0.125
- linear_gate: bfloat16 [2048, 1024], P(('sp', 'tp'), 'fs'), may hold values from -0.125 to 0.125
- decay_bias: float32 [512], P('fs'), may hold values from 2 to 5.5
- norm_gain: float32 [256], replicated, may hold values from 0.1 to 1.9
- window_query: bfloat16 [2048, 1024], P(('sp', 'tp'), 'fs'), may hold values from -0.125 to 0.125
- window_key: bfloat16 [2048, 256], P(('sp', 'tp'), 'fs'), may hold values from -0.125 to 0.125
- window_value: bfloat16 [2048, 256], P(('sp', 'tp'), 'fs'), may hold values from -0.5 to 0.5
- sink_logit: float32 [16], P('fs'), may hold values from 3 to 7
- linear_output: bfloat16 [1024, 2048], P('fs'), may hold values from -0.1875 to 0.1875
- window_output: bfloat16 [1024, 2048], P('fs'), may hold values from -0.1875 to 0.1875
Outputs:
- mixed: bfloat16 [8, 768, 2048], P(('fs', 'tp'), 'sp')
The draws below stay inside these ranges and needn't reach their ends.
All inputs are finite; a program needn't handle non-finite values.
Results may differ from the reference program's by a relative error of at most 0.025.
Values may be sent and summed in bfloat16 or wider, within the bound.
A program may use at most 64 MiB of HBM per device.

```python
import jax
import jax.numpy as jnp
from jax import lax

D = 2048
GLA_HEADS = 4
GLA_KEY = 128
GLA_VALUE = 256
SWA_HEADS = 16
KV_HEADS = 4
HEAD_DIM = 64
WINDOW = 128
BLOCK = 32
SEQ = 768
BATCH = 8
GATE_TAU = 48


def shard_levels(own_key, dims, pieces, least, high):
    loudness = 1.0
    for dim, shards_of in pieces:
        heights = jax.random.uniform(jax.random.fold_in(jax.random.fold_in(own_key, 6), dim), (shards_of,), jnp.float32, least / len(pieces), high / len(pieces))
        loudness = loudness * jnp.repeat(jnp.exp(heights), dims[dim] // shards_of).reshape((-1,) + (1,) * (len(dims) - 1 - dim))
    return loudness


def bell_draw(own_key, shape, scale, most, cuts=(), kind=jnp.bfloat16):
    result = scale * jax.random.normal(own_key, shape, jnp.float32)
    if cuts:
        result = result * shard_levels(own_key, shape, cuts, -0.22, 0.18)
    return jnp.clip(result, -most, most).astype(kind)


def setup_inputs(seed: int = 0) -> dict:
    arg_keys = jax.random.split(jax.random.key(seed), 15)
    return {
        "tokens": bell_draw(arg_keys[0], (BATCH, SEQ, D), 1.0, 6.0, ((0, 8), (1, 4))),
        "linear_query": bell_draw(arg_keys[1], (D, GLA_HEADS * GLA_KEY), D ** -0.5, 0.125, ((0, 8), (1, 4))),
        "linear_key": bell_draw(arg_keys[2], (D, GLA_HEADS * GLA_KEY), D ** -0.5, 0.125, ((0, 8), (1, 4))),
        "linear_decay": bell_draw(arg_keys[3], (D, GLA_HEADS * GLA_KEY), (D // 4) ** -0.5, 0.25, ((0, 8), (1, 4))),
        "linear_value": bell_draw(arg_keys[4], (D, GLA_HEADS * GLA_VALUE), D ** -0.5, 0.125, ((0, 8), (1, 4))),
        "linear_gate": bell_draw(arg_keys[5], (D, GLA_HEADS * GLA_VALUE), D ** -0.5, 0.125, ((0, 8), (1, 4))),
        "decay_bias": jnp.clip(2.0 + 3.5 * jax.random.uniform(arg_keys[6], (GLA_HEADS * GLA_KEY,), jnp.float32) ** shard_levels(arg_keys[6], (GLA_HEADS * GLA_KEY,), ((0, 4),), -0.2, 0.2), 2.0, 5.5),
        "norm_gain": jnp.clip(1.0 + 0.18 * jax.random.normal(arg_keys[7], (GLA_VALUE,), jnp.float32), 0.1, 1.9),
        "window_query": bell_draw(arg_keys[8], (D, SWA_HEADS * HEAD_DIM), D ** -0.5, 0.125, ((0, 8), (1, 4))),
        "window_key": bell_draw(arg_keys[9], (D, KV_HEADS * HEAD_DIM), D ** -0.5, 0.125, ((0, 8), (1, 4))),
        "window_value": bell_draw(arg_keys[10], (D, KV_HEADS * HEAD_DIM), (D // 16) ** -0.5, 0.5, ((0, 8), (1, 4))),
        "sink_logit": jnp.clip(3.0 + 4.0 * jax.random.uniform(arg_keys[11], (SWA_HEADS,), jnp.float32) ** shard_levels(arg_keys[11], (SWA_HEADS,), ((0, 4),), -0.2, 0.2), 3.0, 7.0),
        "linear_output": bell_draw(arg_keys[12], (GLA_HEADS * GLA_VALUE, D), (GLA_HEADS * GLA_VALUE) ** -0.5, 0.1875, ((0, 4),)),
        "window_output": bell_draw(arg_keys[13], (SWA_HEADS * HEAD_DIM, D), (SWA_HEADS * HEAD_DIM) ** -0.5, 0.1875, ((0, 4),)),
    }


norm_epsilon = 1e-05
highest = lax.Precision.HIGHEST

def project(inputs, weight):
    flat_rows = inputs.reshape(-1, inputs.shape[-1])
    product = jnp.dot(flat_rows, weight, preferred_element_type=jnp.float32).astype(jnp.bfloat16)
    return product.reshape(inputs.shape[:-1] + (weight.shape[1],))

def forget_blocks(queries, key_rows, value_rows, forget_logs, block_len):
    batch_size, length, head_count, key_dim = queries.shape
    value_dim = value_rows.shape[-1]
    block_count = length // block_len

    def to_blocks(tensor):
        return tensor.reshape(batch_size, block_count, block_len, head_count, tensor.shape[-1]).transpose(1, 0, 3, 2, 4)

    def from_blocks(tensor):
        return tensor.transpose(1, 0, 3, 2, 4).reshape(batch_size, length, head_count, tensor.shape[-1])
    causal = jnp.tril(jnp.ones((block_len, block_len), dtype=bool))

    def advance(carry, block_inputs):
        carry_state, offset = carry
        query_blk, key_blk, value_blk, forget_blk = block_inputs
        within = jnp.cumsum(forget_blk, axis=2)
        carried = jnp.einsum('bhcd,bhde->bhce', query_blk * jnp.exp(within), carry_state, precision=highest)
        spread = within[:, :, :, None, :] - within[:, :, None, :, :]
        decays = jnp.exp(jnp.where(causal[:, :, None], spread, -jnp.inf))
        scores = jnp.einsum('bhijd,bhjd->bhij', query_blk[:, :, :, None, :] * decays, key_blk, precision=highest)
        inside = jnp.einsum('bhij,bhje->bhie', scores, value_blk, precision=highest)
        final_log = within[:, :, -1, :]
        faded = key_blk * jnp.exp(final_log[:, :, None, :] - within)
        new_state = carry_state * jnp.exp(final_log)[:, :, :, None] + jnp.einsum('bhcd,bhce->bhde', faded, value_blk, precision=highest)
        reaching = jnp.exp(offset[:, :, None, :] + within)
        return ((new_state, offset + final_log), (carried + inside, reaching))
    zero_state = jnp.zeros((batch_size, head_count, key_dim, value_dim), jnp.float32)
    zero_offset = jnp.zeros((batch_size, head_count, key_dim), jnp.float32)
    blocked = (to_blocks(queries), to_blocks(key_rows), to_blocks(value_rows), to_blocks(forget_logs))
    finals, produced = lax.scan(advance, (zero_state, zero_offset), blocked)
    return (from_blocks(produced[0]), from_blocks(produced[1]), finals[0], finals[1])

def finish_linear(state_rows, gate_rows, norm_gain):
    scaled = state_rows * lax.rsqrt(lax.optimization_barrier(jnp.mean(jnp.square(state_rows), axis=-1, keepdims=True)) + norm_epsilon)
    gated = scaled * norm_gain.astype(jnp.float32) * jax.nn.silu(gate_rows.astype(jnp.float32))
    return gated.reshape(state_rows.shape[0], state_rows.shape[1], -1).astype(jnp.bfloat16)

def window_attend(queries, key_rows, value_rows, sink_logit, query_first, window_len, block_len):
    batch_size, length, query_heads, head_dim = queries.shape
    prior_rows = key_rows.shape[1] - length
    kv_heads = key_rows.shape[2]
    group_size = query_heads // kv_heads
    block_count = length // block_len
    span_len = window_len + block_len
    grouped = queries.reshape(batch_size, block_count, block_len, kv_heads, group_size, head_dim)
    sink_grid = sink_logit.astype(jnp.float32).reshape(kv_heads, group_size)[None, :, :, None, None]

    def attend(block_number):
        query_blk = lax.dynamic_index_in_dim(grouped, block_number, 1, keepdims=False)
        start_row = block_number * block_len + prior_rows - window_len
        key_blk = lax.dynamic_slice_in_dim(key_rows, start_row, span_len, 1)
        value_blk = lax.dynamic_slice_in_dim(value_rows, start_row, span_len, 1)
        scores = jnp.einsum('bqhgd,bkhd->bhgqk', query_blk, key_blk, precision=highest) * head_dim ** (-0.5)
        query_pos = query_first + block_number * block_len + jnp.arange(block_len, dtype=jnp.int32)
        key_pos = query_first - prior_rows + start_row + jnp.arange(span_len, dtype=jnp.int32)
        distance = query_pos[:, None] - key_pos[None, :]
        allowed = (distance >= 0) & (distance < window_len) & (key_pos[None, :] >= 0)
        scores = jnp.where(allowed, scores, -jnp.inf)
        highest_score = jnp.maximum(lax.optimization_barrier(jnp.max(scores, axis=-1, keepdims=True)), sink_grid)
        weights = jnp.exp(scores - highest_score)
        normaliser = lax.optimization_barrier(jnp.sum(weights, axis=-1, keepdims=True)) + jnp.exp(sink_grid - highest_score)
        return jnp.einsum('bhgqk,bkhd->bqhgd', weights / normaliser, value_blk, precision=highest)
    blocks_out = lax.map(attend, jnp.arange(block_count, dtype=jnp.int32))
    return blocks_out.transpose(1, 0, 2, 3, 4, 5).reshape(batch_size, length, query_heads * head_dim)

def reference(tokens, linear_query, linear_key, linear_decay, linear_value, linear_gate, decay_bias, norm_gain, window_query, window_key, window_value, sink_logit, linear_output, window_output):
    batch_size, length = (tokens.shape[0], tokens.shape[1])
    state_query = project(tokens, linear_query).astype(jnp.float32).reshape(batch_size, length, GLA_HEADS, GLA_KEY) * GLA_KEY ** (-0.5)
    state_key = project(tokens, linear_key).astype(jnp.float32).reshape(batch_size, length, GLA_HEADS, GLA_KEY)
    decay_input = project(tokens, linear_decay).astype(jnp.float32).reshape(batch_size, length, GLA_HEADS, GLA_KEY)
    state_value = project(tokens, linear_value).astype(jnp.float32).reshape(batch_size, length, GLA_HEADS, GLA_VALUE)
    state_gate = project(tokens, linear_gate).reshape(batch_size, length, GLA_HEADS, GLA_VALUE)
    forget_logs = jax.nn.log_sigmoid(decay_input + decay_bias.astype(jnp.float32).reshape(GLA_HEADS, GLA_KEY)) / GATE_TAU
    state_rows = forget_blocks(state_query, state_key, state_value, forget_logs, BLOCK)[0]
    linear_rows = finish_linear(state_rows, state_gate, norm_gain)
    local_query = project(tokens, window_query).astype(jnp.float32).reshape(batch_size, length, SWA_HEADS, HEAD_DIM)
    local_key = project(tokens, window_key).astype(jnp.float32).reshape(batch_size, length, KV_HEADS, HEAD_DIM)
    local_value = project(tokens, window_value).astype(jnp.float32).reshape(batch_size, length, KV_HEADS, HEAD_DIM)
    padding = ((0, 0), (WINDOW, 0), (0, 0), (0, 0))
    padded_keys = jnp.pad(local_key, padding)
    padded_values = jnp.pad(local_value, padding)
    window_rows = window_attend(local_query, padded_keys, padded_values, sink_logit, 0, WINDOW, BLOCK).astype(jnp.bfloat16)
    linear_part = jnp.dot(linear_rows.reshape(-1, GLA_HEADS * GLA_VALUE), linear_output, preferred_element_type=jnp.float32)
    window_part = jnp.dot(window_rows.reshape(-1, SWA_HEADS * HEAD_DIM), window_output, preferred_element_type=jnp.float32)
    mixed = (linear_part + window_part).astype(jnp.bfloat16)
    return mixed.reshape(batch_size, length, D)
```

```python
import functools

import jax
import jax.numpy as jnp
from jax import lax
from jax.experimental import pallas as pl
from jax.experimental.pallas import tpu as pltpu
from jax.sharding import PartitionSpec as P

GLA_KEY = 128
GLA_VALUE = 256
HEAD_DIM = 64
WINDOW = 128

norm_epsilon = 1e-05
MESH = pl.DeviceIdType.MESH
f32, bf16 = jnp.float32, jnp.bfloat16


def dot(a, b):
    return jnp.dot(a, b, preferred_element_type=f32)


def dot_t(a, b):
    return lax.dot_general(a, b, (((1,), (1,)), ((), ())), preferred_element_type=f32)


def dot_rows(a, b):
    return lax.dot_general(a, b, (((0,), (0,)), ((), ())), preferred_element_type=f32)


def kernel(
    NZ, NF, NT, levels,
    tok, w1, w2, w3, bias, gain, sink, out_w,
    out,
    toks, W1, W2, W3, sums, fhi, flo, kkey, val, kvbuf, qs, oacc, state_in, state_out,
    rows, part, rbuf,
    loc_sem, wsend, wrecv, fsend, frecv, tsend, trecv, ssend, srecv, hsend, hrecv, psend, precv,
):
    z, f, t = lax.axis_index("sp"), lax.axis_index("fs"), lax.axis_index("tp")
    length = tok.shape[0]
    tau = NZ * length // 16

    barrier = pltpu.get_barrier_semaphore()
    for d in range(1, NZ):
        pl.semaphore_signal(barrier, inc=1, device_id={"sp": lax.rem(z + d, NZ)}, device_id_type=MESH)
    for d in range(1, NF):
        pl.semaphore_signal(barrier, inc=1, device_id={"fs": lax.rem(f + d, NF)}, device_id_type=MESH)
    for d in range(1, NT):
        pl.semaphore_signal(barrier, inc=1, device_id={"tp": lax.rem(t + d, NT)}, device_id_type=MESH)
    pl.semaphore_wait(barrier, NZ + NF + NT - 3)

    own = z * NT + t
    groups = ((w1, W1), (w2, W2), (w3, W3))

    def token_copy(d):
        return pltpu.make_async_remote_copy(
            src_ref=tok, dst_ref=toks.at[f], send_sem=tsend.at[d], recv_sem=trecv.at[d],
            device_id={"fs": lax.rem(f + d, NF)}, device_id_type=MESH)

    def weight_copy(g, d):
        src, dst = groups[g]
        return pltpu.make_async_remote_copy(
            src_ref=src, dst_ref=dst.at[own], send_sem=wsend.at[g, d], recv_sem=wrecv.at[g, d],
            device_id={"sp": lax.rem(z + d, NZ)}, device_id_type=MESH)

    def forward_copy(g, d, e):
        src, dst = groups[g]
        slot = lax.rem(z - d + NZ, NZ) * NT + t
        return pltpu.make_async_remote_copy(
            src_ref=src if d == 0 else dst.at[slot], dst_ref=dst.at[slot],
            send_sem=fsend.at[g, d, e], recv_sem=frecv.at[g, d, e],
            device_id={"tp": lax.rem(t + e, NT)}, device_id_type=MESH)

    for d in range(1, NF):
        token_copy(d).start()
    for g in range(3):
        for d in range(1, NZ):
            weight_copy(g, d).start()
        for e in range(1, NT):
            forward_copy(g, 0, e).start()
    local = [pltpu.make_async_copy(tok, toks.at[f], loc_sem.at[0])]
    for g in range(3):
        local.append(pltpu.make_async_copy(groups[g][0], groups[g][1].at[own], loc_sem.at[1 + g]))
    for c in local:
        c.start()

    i = lax.broadcasted_iota(jnp.int32, (length, length), 0)
    s = lax.broadcasted_iota(jnp.int32, (length, length), 1)
    for n, h in enumerate(levels):
        ref = (i & ~(2 * h - 1)) + h - 1
        later = (i & h) != 0
        low = jnp.where(later, ref, i)
        high = jnp.where(later, i, ref)
        sums[n] = jnp.where((s > low) & (s <= high), 1.0, 0.0).astype(bf16)
    sums[len(levels)] = jnp.where(s <= i, 1.0, 0.0).astype(bf16)
    sums[len(levels) + 1] = jnp.where(s > i, 1.0, 0.0).astype(bf16)

    @pl.when(z == 0)
    def _():
        state_in[...] = jnp.zeros_like(state_in)
        kvbuf[:, 0:WINDOW, :] = jnp.zeros((NF, WINDOW, kvbuf.shape[2]), bf16)

    for c in local:
        c.wait()

    def arrive(g):
        for d in range(1, NZ):
            weight_copy(g, d).wait_recv()
            for e in range(1, NT):
                forward_copy(g, d, e).start()
        for d in range(NZ):
            for e in range(1, NT):
                forward_copy(g, d, e).wait_recv()

    def log_sum(n, b):
        m = sums[n]
        return dot(m, fhi[b]) + dot(m, flo[b])

    depth = tok.shape[1]
    arrive(0)
    for d in range(1, NF):
        token_copy(d).wait_recv()

    @pl.loop(0, NF)
    def _(b):
        p = dot(toks[b], W1[...].reshape(depth, -1)).astype(bf16)
        x = p[:, :GLA_KEY].astype(f32) + bias[...]
        forget = (jnp.minimum(x, 0.0) - jnp.log1p(jnp.exp(-jnp.abs(x)))) / tau
        hi = forget.astype(bf16)
        fhi[b] = hi
        flo[b] = (forget - hi.astype(f32)).astype(bf16)
        kkey[b] = p[:, GLA_KEY:2 * GLA_KEY]
        val[b] = p[:, 2 * GLA_KEY:2 * GLA_KEY + GLA_VALUE]
        kvbuf[b, WINDOW:, :] = p[:, 2 * GLA_KEY + GLA_VALUE:]

    def halo_copy():
        return pltpu.make_async_remote_copy(
            src_ref=kvbuf.at[:, pl.ds(length, WINDOW)], dst_ref=kvbuf.at[:, pl.ds(0, WINDOW)],
            send_sem=hsend, recv_sem=hrecv, device_id={"sp": lax.rem(z + 1, NZ)}, device_id_type=MESH)

    def state_copy(b):
        return pltpu.make_async_remote_copy(
            src_ref=state_out.at[b], dst_ref=state_in.at[b],
            send_sem=ssend.at[b], recv_sem=srecv.at[b],
            device_id={"sp": lax.rem(z + 1, NZ)}, device_id_type=MESH)

    @pl.when(z < NZ - 1)
    def _():
        halo_copy().start()

    @pl.loop(0, NF)
    def _(b):
        faded = (kkey[b].astype(f32) * jnp.exp(log_sum(len(levels) + 1, b))).astype(bf16)
        local_state = dot_rows(faded, val[b])
        ones = jnp.ones((length, GLA_VALUE), bf16)
        decay = jnp.exp(dot_rows(fhi[b], ones) + dot_rows(flo[b], ones))

        @pl.when(z > 0)
        def _():
            state_copy(b).wait_recv()

        @pl.when(z < NZ - 1)
        def _():
            state_out[b] = (state_in[b].astype(f32) * decay + local_state).astype(bf16)
            state_copy(b).start()

    arrive(1)

    @pl.when(z > 0)
    def _():
        halo_copy().wait_recv()

    span = length + WINDOW
    row = lax.broadcasted_iota(jnp.int32, (length, span), 0)
    col = lax.broadcasted_iota(jnp.int32, (length, span), 1)
    distance = row - col + WINDOW
    heads = sink.shape[1]
    wq = heads * HEAD_DIM

    @pl.loop(0, NF)
    def _(b):
        p = dot(toks[b], W2[...].reshape(depth, -1)).astype(bf16)
        allowed = (distance >= 0) & (distance < WINDOW) & ((col >= WINDOW) | (z > 0))
        kv = kvbuf[b]
        k, v = kv[:, :HEAD_DIM], kv[:, HEAD_DIM:]
        heads_out = []
        for j in range(heads):
            score = dot_t(p[:, j * HEAD_DIM:(j + 1) * HEAD_DIM], k) * HEAD_DIM ** -0.5
            score = jnp.where(allowed, score, -jnp.inf)
            sk = sink[0:1, j:j + 1]
            top = jnp.maximum(jnp.max(score, axis=1, keepdims=True), sk)
            e = jnp.exp(score - top)
            total = jnp.sum(e, axis=1, keepdims=True) + jnp.exp(sk - top)
            heads_out.append((dot(e.astype(bf16), v) / total).astype(bf16))
        rows[b, :, GLA_VALUE:] = jnp.concatenate(heads_out, axis=1)
        q = p[:, wq:].astype(f32) * GLA_KEY ** -0.5
        k = kkey[b].astype(f32)
        v = val[b]
        ri = lax.broadcasted_iota(jnp.int32, (length, length), 0)
        ci = lax.broadcasted_iota(jnp.int32, (length, length), 1)
        rk = lax.broadcasted_iota(jnp.int32, (length, GLA_KEY), 0)
        scores = jnp.where(ri == ci, dot_t(q.astype(bf16), kkey[b]), 0.0)
        for n, h in enumerate(levels):
            decay = jnp.exp(log_sum(n, b))
            later = (rk & h) != 0
            qh = jnp.where(later, q * decay, 0.0).astype(bf16)
            kh = jnp.where(later, 0.0, k * decay).astype(bf16)
            same = (ri & ~(2 * h - 1)) == (ci & ~(2 * h - 1))
            scores = scores + jnp.where(same, dot_t(qh, kh), 0.0)
        reach = (q * jnp.exp(log_sum(len(levels), b))).astype(bf16)
        oacc[b] = dot(scores.astype(bf16), v) + dot(reach, state_in[b])

    arrive(2)

    def part_copy(d):
        return pltpu.make_async_remote_copy(
            src_ref=part.at[d], dst_ref=rbuf.at[d], send_sem=psend.at[d], recv_sem=precv.at[d],
            device_id={"fs": lax.rem(f + d, NF)}, device_id_type=MESH)

    @pl.loop(1, NF + 1)
    def _(step):
        b = lax.rem(f + step, NF)
        gate = dot(toks[b], W3[...].reshape(depth, -1)).astype(bf16).astype(f32)
        o = oacc[b]
        scaled = o * lax.rsqrt(jnp.mean(o * o, axis=1, keepdims=True) + norm_epsilon)
        rows[b, :, :GLA_VALUE] = (scaled * gain[...] * (gate / (1.0 + jnp.exp(-gate)))).astype(bf16)
        y = dot(rows[b], out_w[...])

        @pl.when(step < NF)
        def _():
            part[step] = y.astype(bf16)
            part_copy(step).start()

        @pl.when(step == NF)
        def _():
            acc = y
            for d in range(1, NF):
                part_copy(d).wait_recv()
                acc = acc + rbuf[d].astype(f32)
            out[...] = acc.astype(bf16)

    for d in range(1, NF):
        token_copy(d).wait_send()
        part_copy(d).wait_send()
    for g in range(3):
        for d in range(1, NZ):
            weight_copy(g, d).wait_send()
        for d in range(NZ):
            for e in range(1, NT):
                forward_copy(g, d, e).wait_send()

    @pl.when(z < NZ - 1)
    def _():
        halo_copy().wait_send()
        for b in range(NF):
            state_copy(b).wait_send()


def shards(
    NZ, NF, NT,
    tokens, linear_query, linear_key, linear_decay, linear_value, linear_gate, decay_bias,
    norm_gain, window_query, window_key, window_value, sink_logit, linear_output, window_output,
):
    _, length, depth = tokens.shape
    w1 = jnp.concatenate([linear_decay, linear_key, linear_value, window_key, window_value], axis=1)
    w2 = jnp.concatenate([window_query, linear_query], axis=1)
    w3 = linear_gate
    out_w = jnp.concatenate([linear_output, window_output], axis=0)
    kb = w1.shape[0]
    n = NZ * NT
    levels = []
    h = 1
    while h < length:
        levels.append(h)
        h *= 2
    vm = pltpu.VMEM
    dma = pltpu.SemaphoreType.DMA
    kv_width = window_key.shape[1] + window_value.shape[1]
    out_rows = out_w.shape[0]
    result = pl.pallas_call(
        functools.partial(kernel, NZ, NF, NT, tuple(levels)),
        out_shape=jax.ShapeDtypeStruct((length, depth), bf16),
        in_specs=[pl.BlockSpec(memory_space=vm)] * 8,
        out_specs=pl.BlockSpec(memory_space=vm),
        scratch_shapes=[
            vm((NF, length, depth), bf16),
            vm((n, kb, w1.shape[1]), bf16),
            vm((n, kb, w2.shape[1]), bf16),
            vm((n, kb, w3.shape[1]), bf16),
            vm((len(levels) + 2, length, length), bf16),
            vm((NF, length, GLA_KEY), bf16),
            vm((NF, length, GLA_KEY), bf16),
            vm((NF, length, GLA_KEY), bf16),
            vm((NF, length, GLA_VALUE), bf16),
            vm((NF, length + WINDOW, kv_width), bf16),
            vm((8, 128), f32),
            vm((NF, length, GLA_VALUE), f32),
            vm((NF, GLA_KEY, GLA_VALUE), bf16),
            vm((NF, GLA_KEY, GLA_VALUE), bf16),
            vm((NF, length, out_rows), bf16),
            vm((NF, length, depth), bf16),
            vm((NF, length, depth), bf16),
            dma((4,)),
            dma((3, NZ)), dma((3, NZ)),
            dma((3, NZ, NT)), dma((3, NZ, NT)),
            dma((NF,)), dma((NF,)),
            dma((NF,)), dma((NF,)),
            dma, dma,
            dma((NF,)), dma((NF,)),
        ],
        compiler_params=pltpu.CompilerParams(
            collective_id=0, has_side_effects=True, vmem_limit_bytes=60 * 1024 * 1024),
        name="layer",
    )(tokens[0], w1, w2, w3, decay_bias[None], norm_gain[None], sink_logit[None], out_w)
    return result[None]


def solution(mesh):
    shape = mesh.shape
    return jax.shard_map(
        functools.partial(shards, shape["sp"], shape["fs"], shape["tp"]),
        mesh=mesh,
        in_specs=(
            P(("fs", "tp"), "sp", None),
            P(("sp", "tp"), "fs"),
            P(("sp", "tp"), "fs"),
            P(("sp", "tp"), "fs"),
            P(("sp", "tp"), "fs"),
            P(("sp", "tp"), "fs"),
            P("fs"),
            P(),
            P(("sp", "tp"), "fs"),
            P(("sp", "tp"), "fs"),
            P(("sp", "tp"), "fs"),
            P("fs"),
            P("fs", None),
            P("fs", None),
        ),
        out_specs=P(("fs", "tp"), "sp", None),
        check_vma=False,
    )
```

```python
import functools

import jax
import jax.numpy as jnp
from jax import lax
from jax.experimental import pallas as pl
from jax.experimental.pallas import tpu as pltpu
from jax.sharding import PartitionSpec as P

GLA_KEY = 128
GLA_VALUE = 256
HEAD_DIM = 64
WINDOW = 128

norm_epsilon = 1e-05
MESH = pl.DeviceIdType.MESH
f32, bf16 = jnp.float32, jnp.bfloat16


def dot(a, b):
    return jnp.dot(a, b, preferred_element_type=f32)


def dot_t(a, b):
    return lax.dot_general(a, b, (((1,), (1,)), ((), ())), preferred_element_type=f32)


def dot_rows(a, b):
    return lax.dot_general(a, b, (((0,), (0,)), ((), ())), preferred_element_type=f32)


def kernel(
    NZ, NF, NT, levels, places,
    tok, decay_w, key_w, query_w, value_w, wquery_w, wkv_w, gate_w, bias, gain, sink, lin_w, win_w,
    out,
    toks, W1, W2, W3, out_w, sums, fhi, flo, kkey, val, kvbuf, qs, wqs, reach, oacc, loc_state, loc_decay,
    state_in, state_out, rows, part, rx, ry, dA, dB,
    loc_sem, wsend, wrecv, osend, orecv, fsend, frecv, tsend, trecv, ssend, srecv, hsend, hrecv, psend, precv,
):
    z, f, t = lax.axis_index("sp"), lax.axis_index("fs"), lax.axis_index("tp")
    length, depth = tok.shape[1:]
    half = length // 2
    tau = NZ * length // 16
    fx = f + 1 - 2 * lax.rem(f, 2)
    fy = lax.rem(f + 2, 4)
    fd = 3 - f

    barrier = pltpu.get_barrier_semaphore()
    for d in range(1, NZ):
        pl.semaphore_signal(barrier, inc=1, device_id={"sp": lax.rem(z + d, NZ)}, device_id_type=MESH)
    for peer in (fx, fy):
        pl.semaphore_signal(barrier, inc=1, device_id={"fs": peer}, device_id_type=MESH)
    for d in range(1, NT):
        pl.semaphore_signal(barrier, inc=1, device_id={"tp": lax.rem(t + d, NT)}, device_id_type=MESH)
    pl.semaphore_wait(barrier, NZ + NT)

    own = z * NT + t
    buffers = (W1, W2, W3)
    sources = ((decay_w, key_w, query_w, value_w), (wquery_w, wkv_w), (gate_w,))
    pieces = []
    for g in range(3):
        for src, col in zip(sources[g], places[g]):
            pieces.append((g, src, buffers[g].at[own, :, pl.ds(col, src.shape[1])]))

    top, low_half = pl.ds(0, half), pl.ds(half, half)

    def remote(src, dst, send, recv, axis, peer):
        return pltpu.make_async_remote_copy(
            src_ref=src, dst_ref=dst, send_sem=send, recv_sem=recv,
            device_id={axis: peer}, device_id_type=MESH)

    def token_copy(n):
        part_rows = (top, low_half, low_half, top)[n] if n < 4 else (top, low_half)[n - 4]
        if n < 4:
            return remote(tok.at[0, part_rows], toks.at[f, part_rows], tsend.at[n], trecv.at[n],
                          "fs", fx if n < 2 else fy)
        slot = (fx, fy)[n - 4]
        return remote(toks.at[slot, part_rows], toks.at[slot, part_rows], tsend.at[n], trecv.at[n],
                      "fs", (fy, fx)[n - 4])

    def weight_copy(n, d):
        g, src, dst = pieces[n]
        return remote(src, dst, wsend.at[n, d], wrecv.at[n, d], "sp", lax.rem(z + d, NZ))

    def own_copy(n, e):
        g, src, dst = pieces[n]
        return remote(src, dst, osend.at[n, e], orecv.at[n, e], "tp", lax.rem(t + e, NT))

    def forward_copy(g, d, e):
        block = buffers[g].at[lax.rem(z - d + NZ, NZ) * NT + t]
        return remote(block, block, fsend.at[g, d, e], frecv.at[g, d, e], "tp", lax.rem(t + e, NT))

    for n in range(4):
        token_copy(n).start()
    for n in range(len(pieces)):
        for d in range(1, NZ):
            weight_copy(n, d).start()
        for e in range(1, NT):
            own_copy(n, e).start()
    local = [
        pltpu.make_async_copy(tok.at[0], toks.at[f], loc_sem.at[0]),
        pltpu.make_async_copy(lin_w, out_w.at[pl.ds(0, lin_w.shape[0])], loc_sem.at[1]),
        pltpu.make_async_copy(win_w, out_w.at[pl.ds(lin_w.shape[0], win_w.shape[0])], loc_sem.at[2]),
    ]
    for n, (g, src, dst) in enumerate(pieces):
        local.append(pltpu.make_async_copy(src, dst, loc_sem.at[3 + n]))
    for c in local:
        c.start()

    i = lax.broadcasted_iota(jnp.int32, (length, length), 0)
    s = lax.broadcasted_iota(jnp.int32, (length, length), 1)
    for n, h in enumerate(levels):
        ref = (i & ~(2 * h - 1)) + h - 1
        later = (i & h) != 0
        low = jnp.where(later, ref, i)
        high = jnp.where(later, i, ref)
        sums[n] = jnp.where((s > low) & (s <= high), 1.0, 0.0).astype(bf16)
    sums[len(levels)] = jnp.where(s <= i, 1.0, 0.0).astype(bf16)
    sums[len(levels) + 1] = jnp.where(s > i, 1.0, 0.0).astype(bf16)

    @pl.when(z == 0)
    def _():
        state_in[...] = jnp.zeros_like(state_in)
        kvbuf[:, 0:WINDOW, :] = jnp.zeros((NF, WINDOW, kvbuf.shape[2]), bf16)

    token_copy(0).wait_recv()
    token_copy(4).start()
    token_copy(2).wait_recv()
    token_copy(5).start()
    for c in local:
        c.wait()

    def arrive(g):
        for d in range(1, NZ):
            for n, piece in enumerate(pieces):
                if piece[0] == g:
                    weight_copy(n, d).wait_recv()
            for e in range(1, NT):
                forward_copy(g, d, e).start()
        for e in range(1, NT):
            for n, piece in enumerate(pieces):
                if piece[0] == g:
                    own_copy(n, e).wait_recv()
            for d in range(1, NZ):
                forward_copy(g, d, e).wait_recv()

    def log_sum(n, b):
        m = sums[n]
        return dot(m, fhi[b]) + dot(m, flo[b])

    def project(buffer, col, width):
        x = toks[...].reshape(NF * length, depth)
        w = buffer[:, :, col:col + width].reshape(depth, width)
        return dot(x, w).astype(bf16).reshape(NF, length, width)

    for n in (1, 3, 4, 5):
        token_copy(n).wait_recv()
    arrive(0)
    pair = project(W1, 0, 2 * GLA_KEY)
    x = pair[:, :, :GLA_KEY].astype(f32) + bias[...]
    forget = (jnp.minimum(x, 0.0) - jnp.log1p(jnp.exp(-jnp.abs(x)))) / tau
    hi = forget.astype(bf16)
    fhi[...] = hi
    flo[...] = (forget - hi.astype(f32)).astype(bf16)
    kkey[...] = pair[:, :, GLA_KEY:]
    rest = project(W1, 2 * GLA_KEY, GLA_KEY + GLA_VALUE)
    qs[...] = rest[:, :, :GLA_KEY]
    val[...] = rest[:, :, GLA_KEY:]

    def halo_copy():
        return remote(kvbuf.at[:, pl.ds(length, WINDOW)], kvbuf.at[:, pl.ds(0, WINDOW)],
                      hsend, hrecv, "sp", lax.rem(z + 1, NZ))

    def state_copy(b):
        return remote(state_out.at[b], state_in.at[b], ssend.at[b], srecv.at[b],
                      "sp", lax.rem(z + 1, NZ))

    @pl.loop(0, NF)
    def _(b):
        faded = (kkey[b].astype(f32) * jnp.exp(log_sum(len(levels) + 1, b))).astype(bf16)
        state = dot_rows(faded, val[b])
        ones = jnp.ones((length, GLA_VALUE), bf16)
        loc_state[b] = state
        loc_decay[b] = jnp.exp(dot_rows(fhi[b], ones) + dot_rows(flo[b], ones))

        @pl.when(z == 0)
        def _():
            state_out[b] = state.astype(bf16)
            state_copy(b).start()

    @pl.loop(0, NF)
    def _(b):
        q = qs[b].astype(f32) * GLA_KEY ** -0.5
        k = kkey[b].astype(f32)
        ri = lax.broadcasted_iota(jnp.int32, (length, length), 0)
        ci = lax.broadcasted_iota(jnp.int32, (length, length), 1)
        rk = lax.broadcasted_iota(jnp.int32, (length, GLA_KEY), 0)
        scores = jnp.where(ri == ci, dot_t(q.astype(bf16), kkey[b]), 0.0)
        for n, h in enumerate(levels):
            decay = jnp.exp(log_sum(n, b))
            later = (rk & h) != 0
            qh = jnp.where(later, q * decay, 0.0).astype(bf16)
            kh = jnp.where(later, 0.0, k * decay).astype(bf16)
            same = (ri & ~(2 * h - 1)) == (ci & ~(2 * h - 1))
            scores = scores + jnp.where(same, dot_t(qh, kh), 0.0)
        reach[b] = (q * jnp.exp(log_sum(len(levels), b))).astype(bf16)
        oacc[b] = dot(scores.astype(bf16), val[b])

        @pl.when((z > 0) & (z < NZ - 1))
        def _():
            state_copy(b).wait_recv()
            state_out[b] = (state_in[b].astype(f32) * loc_decay[b] + loc_state[b]).astype(bf16)
            state_copy(b).start()

    arrive(1)
    heads = sink.shape[1]
    wq = heads * HEAD_DIM
    kvbuf[:, WINDOW:, :] = project(W2, wq, kvbuf.shape[2])

    @pl.when(z < NZ - 1)
    def _():
        halo_copy().start()

    wqs[...] = project(W2, 0, wq)

    @pl.when(z > 0)
    def _():
        halo_copy().wait_recv()

    span = length + WINDOW

    @pl.loop(0, NF)
    def _(b):
        row = lax.broadcasted_iota(jnp.int32, (length, span), 0)
        col = lax.broadcasted_iota(jnp.int32, (length, span), 1)
        distance = row - col + WINDOW
        allowed = (distance >= 0) & (distance < WINDOW) & ((col >= WINDOW) | (z > 0))
        kv = kvbuf[b]
        p = wqs[b]
        k, v = kv[:, :HEAD_DIM], kv[:, HEAD_DIM:]
        heads_out = []
        for j in range(heads):
            score = dot_t(p[:, j * HEAD_DIM:(j + 1) * HEAD_DIM], k) * HEAD_DIM ** -0.5
            score = jnp.where(allowed, score, -jnp.inf)
            sk = sink[0:1, j:j + 1]
            top_score = jnp.maximum(jnp.max(score, axis=1, keepdims=True), sk)
            e = jnp.exp(score - top_score)
            total = jnp.sum(e, axis=1, keepdims=True) + jnp.exp(sk - top_score)
            heads_out.append((dot(e.astype(bf16), v) / total).astype(bf16))
        rows[b, :, GLA_VALUE:] = jnp.concatenate(heads_out, axis=1)

    @pl.when(z == NZ - 1)
    def _():
        for b in range(NF):
            state_copy(b).wait_recv()

    @pl.loop(0, NF)
    def _(b):
        oacc[b] = oacc[b] + dot(reach[b], state_in[b])

    arrive(2)
    gate = project(W3, 0, GLA_VALUE).astype(f32)
    o = oacc[...]
    scaled = o * lax.rsqrt(jnp.mean(o * o, axis=2, keepdims=True) + norm_epsilon)
    rows[:, :, :GLA_VALUE] = (scaled * gain[...] * (gate / (1.0 + jnp.exp(-gate)))).astype(bf16)

    A, B = slice(0, half), slice(half, length)
    part_copies = [
        remote(part.at[0, top], dA, psend.at[0], precv.at[0], "fs", fx),
        remote(part.at[0, low_half], dB, psend.at[1], precv.at[1], "fs", fy),
        remote(part.at[1, top], rx.at[top], psend.at[2], precv.at[2], "fs", fx),
        remote(part.at[2, low_half], ry.at[low_half], psend.at[3], precv.at[3], "fs", fy),
        remote(part.at[1, low_half], rx.at[low_half], psend.at[4], precv.at[4], "fs", fx),
        remote(part.at[2, top], ry.at[top], psend.at[5], precv.at[5], "fs", fy),
    ]
    part[0] = dot(rows[fd], out_w[...]).astype(bf16)
    part_copies[0].start()
    part_copies[1].start()
    part[1, A] = dot(rows[fx, A], out_w[...]).astype(bf16)
    part_copies[2].start()
    part[2, B] = dot(rows[fy, B], out_w[...]).astype(bf16)
    part_copies[3].start()
    yx = dot(rows[fx, B], out_w[...])
    part_copies[1].wait_recv()
    part[1, B] = (yx + dB[...].astype(f32)).astype(bf16)
    part_copies[4].start()
    yy = dot(rows[fy, A], out_w[...])
    part_copies[0].wait_recv()
    part[2, A] = (yy + dA[...].astype(f32)).astype(bf16)
    part_copies[5].start()
    acc = dot(rows[f], out_w[...])
    for n in (2, 3):
        part_copies[n].wait_recv()
    for n in (4, 5):
        part_copies[n].wait_recv()
    out[0] = (acc + rx[...].astype(f32) + ry[...].astype(f32)).astype(bf16)

    for c in part_copies:
        c.wait_send()
    for n in range(6):
        token_copy(n).wait_send()
    for n in range(len(pieces)):
        for d in range(1, NZ):
            weight_copy(n, d).wait_send()
        for e in range(1, NT):
            own_copy(n, e).wait_send()
    for g in range(3):
        for d in range(1, NZ):
            for e in range(1, NT):
                forward_copy(g, d, e).wait_send()

    @pl.when(z < NZ - 1)
    def _():
        halo_copy().wait_send()
        for b in range(NF):
            state_copy(b).wait_send()


def shards(
    NZ, NF, NT,
    tokens, linear_query, linear_key, linear_decay, linear_value, linear_gate, decay_bias,
    norm_gain, window_query, window_key, window_value, sink_logit, linear_output, window_output,
):
    _, length, depth = tokens.shape
    assert NF == 4 and length >= WINDOW
    window_kv = jnp.concatenate([window_key, window_value], axis=1)
    groups = (
        (linear_decay, linear_key, linear_query, linear_value),
        (window_query, window_kv),
        (linear_gate,),
    )
    places, widths = [], []
    for group in groups:
        col, cols = 0, []
        for w in group:
            cols.append(col)
            col += w.shape[1]
        places.append(tuple(cols))
        widths.append(col)
    kb = linear_query.shape[0]
    n = NZ * NT
    levels = []
    h = 1
    while h < length:
        levels.append(h)
        h *= 2
    vm = pltpu.VMEM
    dma = pltpu.SemaphoreType.DMA
    kv_width = window_kv.shape[1]
    out_rows = linear_output.shape[0] + window_output.shape[0]
    anyspec, vspec = pl.BlockSpec(memory_space=pl.ANY), pl.BlockSpec(memory_space=vm)
    return pl.pallas_call(
        functools.partial(kernel, NZ, NF, NT, tuple(levels), tuple(places)),
        out_shape=jax.ShapeDtypeStruct((1, length, depth), bf16),
        in_specs=[anyspec] * 8 + [vspec] * 3 + [anyspec] * 2,
        out_specs=vspec,
        scratch_shapes=[
            vm((NF, length, depth), bf16),
            vm((n, kb, widths[0]), bf16),
            vm((n, kb, widths[1]), bf16),
            vm((n, kb, widths[2]), bf16),
            vm((out_rows, depth), bf16),
            vm((len(levels) + 2, length, length), bf16),
            vm((NF, length, GLA_KEY), bf16),
            vm((NF, length, GLA_KEY), bf16),
            vm((NF, length, GLA_KEY), bf16),
            vm((NF, length, GLA_VALUE), bf16),
            vm((NF, length + WINDOW, kv_width), bf16),
            vm((NF, length, GLA_KEY), bf16),
            vm((NF, length, window_query.shape[1]), bf16),
            vm((NF, length, GLA_KEY), bf16),
            vm((NF, length, GLA_VALUE), f32),
            vm((NF, GLA_KEY, GLA_VALUE), f32),
            vm((NF, GLA_KEY, GLA_VALUE), f32),
            vm((NF, GLA_KEY, GLA_VALUE), bf16),
            vm((NF, GLA_KEY, GLA_VALUE), bf16),
            vm((NF, length, out_rows), bf16),
            vm((3, length, depth), bf16),
            vm((length, depth), bf16),
            vm((length, depth), bf16),
            vm((length // 2, depth), bf16),
            vm((length // 2, depth), bf16),
            dma((10,)),
            dma((7, NZ)), dma((7, NZ)),
            dma((7, NT)), dma((7, NT)),
            dma((3, NZ, NT)), dma((3, NZ, NT)),
            dma((6,)), dma((6,)),
            dma((NF,)), dma((NF,)),
            dma, dma,
            dma((6,)), dma((6,)),
        ],
        compiler_params=pltpu.CompilerParams(
            collective_id=0, has_side_effects=True, vmem_limit_bytes=60 * 1024 * 1024),
        name="layer",
    )(tokens, linear_decay, linear_key, linear_query, linear_value, window_query, window_kv, linear_gate,
      decay_bias[None], norm_gain[None], sink_logit[None], linear_output, window_output)


def solution(mesh):
    shape = mesh.shape
    return jax.shard_map(
        functools.partial(shards, shape["sp"], shape["fs"], shape["tp"]),
        mesh=mesh,
        in_specs=(
            P(("fs", "tp"), "sp", None),
            P(("sp", "tp"), "fs"),
            P(("sp", "tp"), "fs"),
            P(("sp", "tp"), "fs"),
            P(("sp", "tp"), "fs"),
            P(("sp", "tp"), "fs"),
            P("fs"),
            P(),
            P(("sp", "tp"), "fs"),
            P(("sp", "tp"), "fs"),
            P(("sp", "tp"), "fs"),
            P("fs"),
            P("fs", None),
            P("fs", None),
        ),
        out_specs=P(("fs", "tp"), "sp", None),
        check_vma=False,
    )
```

```python
import functools

import jax
import jax.numpy as jnp
from jax import lax
from jax.experimental import pallas as pl
from jax.experimental.pallas import tpu as pltpu
from jax.sharding import PartitionSpec as P

GLA_KEY = 128
GLA_VALUE = 256
HEAD_DIM = 64
WINDOW = 128

norm_epsilon = 1e-05
MESH = pl.DeviceIdType.MESH
f32, bf16 = jnp.float32, jnp.bfloat16


def dot(a, b):
    return jnp.dot(a, b, preferred_element_type=f32)


def dot_t(a, b):
    return lax.dot_general(a, b, (((1,), (1,)), ((), ())), preferred_element_type=f32)


def dot_rows(a, b):
    return lax.dot_general(a, b, (((0,), (0,)), ((), ())), preferred_element_type=f32)


def kernel(
    NZ, NF, NT, levels, places,
    tok, decay_w, key_w, query_w, value_w, wquery_w, wkv_w, gate_w, bias, gain, sink, lin_w, win_w,
    out,
    toks, W1, W2, W3, out_w, sums, fboth, kkey, val, kvbuf, qs, wqs, reach, oacc, loc_state, loc_decay,
    state_in, state_out, rows, part, rx, ry, dA, dB,
    loc_sem, wsend, wrecv, osend, orecv, fsend, frecv, tsend, trecv, ssend, srecv, hsend, hrecv, psend, precv,
):
    z, f, t = lax.axis_index("sp"), lax.axis_index("fs"), lax.axis_index("tp")
    length, depth = tok.shape[1:]
    half = length // 2
    tau = NZ * length // 16
    fx = f + 1 - 2 * lax.rem(f, 2)
    fy = lax.rem(f + 2, 4)
    fd = 3 - f

    barrier = pltpu.get_barrier_semaphore()
    for d in range(1, NZ):
        pl.semaphore_signal(barrier, inc=1, device_id={"sp": lax.rem(z + d, NZ)}, device_id_type=MESH)
    for peer in (fx, fy):
        pl.semaphore_signal(barrier, inc=1, device_id={"fs": peer}, device_id_type=MESH)
    for d in range(1, NT):
        pl.semaphore_signal(barrier, inc=1, device_id={"tp": lax.rem(t + d, NT)}, device_id_type=MESH)
    pl.semaphore_wait(barrier, NZ + NT)

    own = z * NT + t
    buffers = (W1, W2, W3)
    sources = ((decay_w, key_w, query_w, value_w), (wquery_w, wkv_w), (gate_w,))
    pieces = []
    for g in range(3):
        for src, col in zip(sources[g], places[g]):
            pieces.append((g, src, buffers[g].at[own, :, pl.ds(col, src.shape[1])]))

    top, low_half = pl.ds(0, half), pl.ds(half, half)

    def remote(src, dst, send, recv, axis, peer):
        return pltpu.make_async_remote_copy(
            src_ref=src, dst_ref=dst, send_sem=send, recv_sem=recv,
            device_id={axis: peer}, device_id_type=MESH)

    def token_copy(n):
        part_rows = (top, low_half, low_half, top)[n] if n < 4 else (top, low_half)[n - 4]
        if n < 4:
            return remote(tok.at[0, part_rows], toks.at[f, part_rows], tsend.at[n], trecv.at[n],
                          "fs", fx if n < 2 else fy)
        slot = (fx, fy)[n - 4]
        return remote(toks.at[slot, part_rows], toks.at[slot, part_rows], tsend.at[n], trecv.at[n],
                      "fs", (fy, fx)[n - 4])

    def weight_copy(n, d):
        g, src, dst = pieces[n]
        return remote(src, dst, wsend.at[n, d], wrecv.at[n, d], "sp", lax.rem(z + d, NZ))

    def own_copy(n, e):
        g, src, dst = pieces[n]
        return remote(src, dst, osend.at[n, e], orecv.at[n, e], "tp", lax.rem(t + e, NT))

    def forward_copy(g, d, e):
        block = buffers[g].at[lax.rem(z - d + NZ, NZ) * NT + t]
        return remote(block, block, fsend.at[g, d, e], frecv.at[g, d, e], "tp", lax.rem(t + e, NT))

    for n in range(4):
        token_copy(n).start()
    for n in range(len(pieces)):
        for d in range(1, NZ):
            weight_copy(n, d).start()
        for e in range(1, NT):
            own_copy(n, e).start()
    local = [
        pltpu.make_async_copy(tok.at[0], toks.at[f], loc_sem.at[0]),
        pltpu.make_async_copy(lin_w, out_w.at[pl.ds(0, lin_w.shape[0])], loc_sem.at[1]),
        pltpu.make_async_copy(win_w, out_w.at[pl.ds(lin_w.shape[0], win_w.shape[0])], loc_sem.at[2]),
    ]
    for n, (g, src, dst) in enumerate(pieces):
        local.append(pltpu.make_async_copy(src, dst, loc_sem.at[3 + n]))
    for c in local:
        c.start()

    i = lax.broadcasted_iota(jnp.int32, (length, length), 0)
    s = lax.broadcasted_iota(jnp.int32, (length, length), 1)
    for n, h in enumerate(levels):
        ref = (i & ~(2 * h - 1)) + h - 1
        later = (i & h) != 0
        low = jnp.where(later, ref, i)
        high = jnp.where(later, i, ref)
        sums[n] = jnp.where((s > low) & (s <= high), 1.0, 0.0).astype(bf16)
    sums[len(levels)] = jnp.where(s <= i, 1.0, 0.0).astype(bf16)
    sums[len(levels) + 1] = jnp.where(s > i, 1.0, 0.0).astype(bf16)

    @pl.when(z == 0)
    def _():
        state_in[...] = jnp.zeros_like(state_in)
        kvbuf[:, 0:WINDOW, :] = jnp.zeros((NF, WINDOW, kvbuf.shape[2]), bf16)

    token_copy(0).wait_recv()
    token_copy(4).start()
    token_copy(2).wait_recv()
    token_copy(5).start()
    for c in local:
        c.wait()

    def arrive(g):
        for d in range(1, NZ):
            for n, piece in enumerate(pieces):
                if piece[0] == g:
                    weight_copy(n, d).wait_recv()
            for e in range(1, NT):
                forward_copy(g, d, e).start()
        for e in range(1, NT):
            for n, piece in enumerate(pieces):
                if piece[0] == g:
                    own_copy(n, e).wait_recv()
            for d in range(1, NZ):
                forward_copy(g, d, e).wait_recv()

    def log_sum(n, b):
        both = dot(sums[n], fboth[b])
        return both[:, :GLA_KEY] + both[:, GLA_KEY:]

    def project(buffer, col, width):
        x = toks[...].reshape(NF * length, depth)
        w = buffer[:, :, col:col + width].reshape(depth, width)
        return dot(x, w).astype(bf16).reshape(NF, length, width)

    for n in (1, 3, 4, 5):
        token_copy(n).wait_recv()
    arrive(0)
    pair = project(W1, 0, 2 * GLA_KEY)
    x = pair[:, :, :GLA_KEY].astype(f32) + bias[...]
    forget = (jnp.minimum(x, 0.0) - jnp.log1p(jnp.exp(-jnp.abs(x)))) / tau
    hi = forget.astype(bf16)
    fboth[:, :, :GLA_KEY] = hi
    fboth[:, :, GLA_KEY:] = (forget - hi.astype(f32)).astype(bf16)
    kkey[...] = pair[:, :, GLA_KEY:]
    rest = project(W1, 2 * GLA_KEY, GLA_KEY + GLA_VALUE)
    qs[...] = rest[:, :, :GLA_KEY]
    val[...] = rest[:, :, GLA_KEY:]

    def halo_copy():
        return remote(kvbuf.at[:, pl.ds(length, WINDOW)], kvbuf.at[:, pl.ds(0, WINDOW)],
                      hsend, hrecv, "sp", lax.rem(z + 1, NZ))

    def state_copy(b):
        return remote(state_out.at[b], state_in.at[b], ssend.at[b], srecv.at[b],
                      "sp", lax.rem(z + 1, NZ))

    @pl.loop(0, NF)
    def _(b):
        faded = (kkey[b].astype(f32) * jnp.exp(log_sum(len(levels) + 1, b))).astype(bf16)
        state = dot_rows(faded, val[b])
        ones = jnp.ones((length, GLA_VALUE), bf16)
        loc_state[b] = state
        loc_decay[b] = jnp.exp(dot_rows(fboth[b, :, :GLA_KEY], ones) + dot_rows(fboth[b, :, GLA_KEY:], ones))

        @pl.when(z == 0)
        def _():
            state_out[b] = state.astype(bf16)
            state_copy(b).start()

    def pass_state(b):
        @pl.when((z > 0) & (z < NZ - 1))
        def _():
            state_copy(b).wait_recv()
            state_out[b] = (state_in[b].astype(f32) * loc_decay[b] + loc_state[b]).astype(bf16)
            state_copy(b).start()

    def inside(b):
        q = qs[b].astype(f32) * GLA_KEY ** -0.5
        k = kkey[b].astype(f32)
        ri = lax.broadcasted_iota(jnp.int32, (length, length), 0)
        ci = lax.broadcasted_iota(jnp.int32, (length, length), 1)
        rk = lax.broadcasted_iota(jnp.int32, (length, GLA_KEY), 0)
        scores = jnp.where(ri == ci, dot_t(q.astype(bf16), kkey[b]), 0.0)
        for n, h in enumerate(levels):
            decay = jnp.exp(log_sum(n, b))
            later = (rk & h) != 0
            qh = jnp.where(later, q * decay, 0.0).astype(bf16)
            kh = jnp.where(later, 0.0, k * decay).astype(bf16)
            same = (ri & ~(2 * h - 1)) == (ci & ~(2 * h - 1))
            scores = scores + jnp.where(same, dot_t(qh, kh), 0.0)
        reach[b] = (q * jnp.exp(log_sum(len(levels), b))).astype(bf16)
        return dot(scores.astype(bf16), val[b])

    @pl.loop(0, NF // 2)
    def _(pair_id):
        first, second = inside(2 * pair_id), inside(2 * pair_id + 1)
        oacc[2 * pair_id] = first
        oacc[2 * pair_id + 1] = second
        for b in (2 * pair_id, 2 * pair_id + 1):
            pass_state(b)

    arrive(1)
    heads = sink.shape[1]
    wq = heads * HEAD_DIM
    kvbuf[:, WINDOW:, :] = project(W2, wq, kvbuf.shape[2])

    @pl.when(z < NZ - 1)
    def _():
        halo_copy().start()

    wqs[...] = project(W2, 0, wq)

    @pl.when(z > 0)
    def _():
        halo_copy().wait_recv()

    span = length + WINDOW

    def window(b):
        row = lax.broadcasted_iota(jnp.int32, (length, span), 0)
        col = lax.broadcasted_iota(jnp.int32, (length, span), 1)
        distance = row - col + WINDOW
        allowed = (distance >= 0) & (distance < WINDOW) & ((col >= WINDOW) | (z > 0))
        kv = kvbuf[b]
        p = wqs[b]
        k, v = kv[:, :HEAD_DIM], kv[:, HEAD_DIM:]
        heads_out = []
        for j in range(heads):
            score = dot_t(p[:, j * HEAD_DIM:(j + 1) * HEAD_DIM], k) * HEAD_DIM ** -0.5
            score = jnp.where(allowed, score, -jnp.inf)
            sk = sink[0:1, j:j + 1]
            top_score = jnp.maximum(jnp.max(score, axis=1, keepdims=True), sk)
            e = jnp.exp(score - top_score)
            total = jnp.sum(e, axis=1, keepdims=True) + jnp.exp(sk - top_score)
            heads_out.append((dot(e.astype(bf16), v) / total).astype(bf16))
        return jnp.concatenate(heads_out, axis=1)

    @pl.loop(0, NF // 2)
    def _(pair_id):
        first, second = window(2 * pair_id), window(2 * pair_id + 1)
        rows[2 * pair_id, :, GLA_VALUE:] = first
        rows[2 * pair_id + 1, :, GLA_VALUE:] = second

    @pl.when(z == NZ - 1)
    def _():
        for b in range(NF):
            state_copy(b).wait_recv()

    @pl.loop(0, NF)
    def _(b):
        oacc[b] = oacc[b] + dot(reach[b], state_in[b])

    arrive(2)
    gate = project(W3, 0, GLA_VALUE).astype(f32)
    o = oacc[...]
    scaled = o * lax.rsqrt(jnp.mean(o * o, axis=2, keepdims=True) + norm_epsilon)
    rows[:, :, :GLA_VALUE] = (scaled * gain[...] * (gate / (1.0 + jnp.exp(-gate)))).astype(bf16)

    A, B = slice(0, half), slice(half, length)
    part_copies = [
        remote(part.at[0, top], dA, psend.at[0], precv.at[0], "fs", fx),
        remote(part.at[0, low_half], dB, psend.at[1], precv.at[1], "fs", fy),
        remote(part.at[1, top], rx.at[top], psend.at[2], precv.at[2], "fs", fx),
        remote(part.at[2, low_half], ry.at[low_half], psend.at[3], precv.at[3], "fs", fy),
        remote(part.at[1, low_half], rx.at[low_half], psend.at[4], precv.at[4], "fs", fx),
        remote(part.at[2, top], ry.at[top], psend.at[5], precv.at[5], "fs", fy),
    ]
    part[0] = dot(rows[fd], out_w[...]).astype(bf16)
    part_copies[0].start()
    part_copies[1].start()
    part[1, A] = dot(rows[fx, A], out_w[...]).astype(bf16)
    part_copies[2].start()
    part[2, B] = dot(rows[fy, B], out_w[...]).astype(bf16)
    part_copies[3].start()
    yx = dot(rows[fx, B], out_w[...])
    part_copies[1].wait_recv()
    part[1, B] = (yx + dB[...].astype(f32)).astype(bf16)
    part_copies[4].start()
    yy = dot(rows[fy, A], out_w[...])
    part_copies[0].wait_recv()
    part[2, A] = (yy + dA[...].astype(f32)).astype(bf16)
    part_copies[5].start()
    acc = dot(rows[f], out_w[...])
    for n in (2, 3):
        part_copies[n].wait_recv()
    for n in (4, 5):
        part_copies[n].wait_recv()
    out[0] = (acc + rx[...].astype(f32) + ry[...].astype(f32)).astype(bf16)

    for c in part_copies:
        c.wait_send()
    for n in range(6):
        token_copy(n).wait_send()
    for n in range(len(pieces)):
        for d in range(1, NZ):
            weight_copy(n, d).wait_send()
        for e in range(1, NT):
            own_copy(n, e).wait_send()
    for g in range(3):
        for d in range(1, NZ):
            for e in range(1, NT):
                forward_copy(g, d, e).wait_send()

    @pl.when(z < NZ - 1)
    def _():
        halo_copy().wait_send()
        for b in range(NF):
            state_copy(b).wait_send()


def shards(
    NZ, NF, NT,
    tokens, linear_query, linear_key, linear_decay, linear_value, linear_gate, decay_bias,
    norm_gain, window_query, window_key, window_value, sink_logit, linear_output, window_output,
):
    _, length, depth = tokens.shape
    assert NF == 4 and length >= WINDOW
    window_kv = jnp.concatenate([window_key, window_value], axis=1)
    groups = (
        (linear_decay, linear_key, linear_query, linear_value),
        (window_query, window_kv),
        (linear_gate,),
    )
    places, widths = [], []
    for group in groups:
        col, cols = 0, []
        for w in group:
            cols.append(col)
            col += w.shape[1]
        places.append(tuple(cols))
        widths.append(col)
    kb = linear_query.shape[0]
    n = NZ * NT
    levels = []
    h = 1
    while h < length:
        levels.append(h)
        h *= 2
    vm = pltpu.VMEM
    dma = pltpu.SemaphoreType.DMA
    kv_width = window_kv.shape[1]
    out_rows = linear_output.shape[0] + window_output.shape[0]
    anyspec, vspec = pl.BlockSpec(memory_space=pl.ANY), pl.BlockSpec(memory_space=vm)
    return pl.pallas_call(
        functools.partial(kernel, NZ, NF, NT, tuple(levels), tuple(places)),
        out_shape=jax.ShapeDtypeStruct((1, length, depth), bf16),
        in_specs=[anyspec] * 8 + [vspec] * 3 + [anyspec] * 2,
        out_specs=vspec,
        scratch_shapes=[
            vm((NF, length, depth), bf16),
            vm((n, kb, widths[0]), bf16),
            vm((n, kb, widths[1]), bf16),
            vm((n, kb, widths[2]), bf16),
            vm((out_rows, depth), bf16),
            vm((len(levels) + 2, length, length), bf16),
            vm((NF, length, 2 * GLA_KEY), bf16),
            vm((NF, length, GLA_KEY), bf16),
            vm((NF, length, GLA_VALUE), bf16),
            vm((NF, length + WINDOW, kv_width), bf16),
            vm((NF, length, GLA_KEY), bf16),
            vm((NF, length, window_query.shape[1]), bf16),
            vm((NF, length, GLA_KEY), bf16),
            vm((NF, length, GLA_VALUE), f32),
            vm((NF, GLA_KEY, GLA_VALUE), f32),
            vm((NF, GLA_KEY, GLA_VALUE), f32),
            vm((NF, GLA_KEY, GLA_VALUE), bf16),
            vm((NF, GLA_KEY, GLA_VALUE), bf16),
            vm((NF, length, out_rows), bf16),
            vm((3, length, depth), bf16),
            vm((length, depth), bf16),
            vm((length, depth), bf16),
            vm((length // 2, depth), bf16),
            vm((length // 2, depth), bf16),
            dma((10,)),
            dma((7, NZ)), dma((7, NZ)),
            dma((7, NT)), dma((7, NT)),
            dma((3, NZ, NT)), dma((3, NZ, NT)),
            dma((6,)), dma((6,)),
            dma((NF,)), dma((NF,)),
            dma, dma,
            dma((6,)), dma((6,)),
        ],
        compiler_params=pltpu.CompilerParams(
            collective_id=0, has_side_effects=True, vmem_limit_bytes=60 * 1024 * 1024),
        name="layer",
    )(tokens, linear_decay, linear_key, linear_query, linear_value, window_query, window_kv, linear_gate,
      decay_bias[None], norm_gain[None], sink_logit[None], linear_output, window_output)


def solution(mesh):
    shape = mesh.shape
    return jax.shard_map(
        functools.partial(shards, shape["sp"], shape["fs"], shape["tp"]),
        mesh=mesh,
        in_specs=(
            P(("fs", "tp"), "sp", None),
            P(("sp", "tp"), "fs"),
            P(("sp", "tp"), "fs"),
            P(("sp", "tp"), "fs"),
            P(("sp", "tp"), "fs"),
            P(("sp", "tp"), "fs"),
            P("fs"),
            P(),
            P(("sp", "tp"), "fs"),
            P(("sp", "tp"), "fs"),
            P(("sp", "tp"), "fs"),
            P("fs"),
            P("fs", None),
            P("fs", None),
        ),
        out_specs=P(("fs", "tp"), "sp", None),
        check_vma=False,
    )
```
